32 devices in a mesh: grp: 2 (over x), st: 4 (over y, core), tp: 4 (over z).
Axes of the slice: x: 2, y: 2, z: 4, core: 2. Of those that a mesh axis runs over, the one named last changes fastest.
Arguments:
- tokens: bfloat16 [4096, 2048], P(('grp', 'st')), parts along dimension 0, may hold values from -6 to 6, as said below
- store: bfloat16 [64, 128, 2048], P(('grp', 'st')), parts along dimension 0, may hold values from -6 to 6, as said below
- passage_ids: int32 [64, 4], P(('grp', 'st')), parts along dimension 0, may hold values from 0 to 31, as said below
- mix_gain: float32 [2048], replicated, may hold values from 0.1 to 1.9
- glu_value: bfloat16 [2048, 1024], P(None, 'tp'), may hold values from -0.125 to 0.125
- glu_gate: bfloat16 [2048, 1024], P(None, 'tp'), may hold values from -0.125 to 0.125
- conv_taps: bfloat16 [31, 1024], P(None, 'tp'), may hold values from -5 to 5
- channel_gain: float32 [1024], P('tp'), may hold values from 0.1 to 1.9
- mix_out: bfloat16 [1024, 2048], P('tp'), may hold values from -0.1875 to 0.1875
- query_gain: float32 [2048], replicated, may hold values from 0.1 to 1.9
- passage_gain: float32 [2048], replicated, may hold values from 0.1 to 1.9
- query_proj: bfloat16 [2048, 2048], P(None, 'tp'), may hold values from -1 to 1
- key_proj: bfloat16 [2048, 2048], P(None, 'tp'), may hold values from -1 to 1
- value_proj: bfloat16 [2048, 2048], P(None, 'tp'), may hold values from -0.125 to 0.125
- attn_out: bfloat16 [2048, 2048], P('tp'), may hold values from -0.125 to 0.125
- blend_gain: float32 [2048], replicated, may hold values from 0.5 to 3
Outputs:
- blended: bfloat16 [4096, 2048], P(('grp', 'st', 'tp')), parts along dimension 0
The draws below stay inside these ranges and needn't reach their ends.
There are 2 independent parts, one for each index of `grp`. The reference program is written for one: setup_inputs(seed, part) draws one part's arguments, and reference() takes and returns one part's arrays. A program takes and returns all parts, laid end to end along the dimension named above; an argument that names none is the same for every part. Nothing has to cross between parts.
Inputs may be any that keep to these rules, and one draw needn't show every extreme that they name: `tokens`: standard normal entries clipped to the range. `store`: standard normal entries clipped to the range. `passage_ids`: passage p is held by index p // 8 of st. The 32 requests of the 8 blocks of one index of st (repeats counted) name at most 16 passages held by any one index of st, and in every draw one index of st receives exactly 16 requests from every index of st.
All inputs are finite; a program needn't handle non-finite values.
Results may differ from the reference program's by a relative error of at most 0.01575.
The reference program's roundings to bfloat16 on the way count: a program that leaves them out, or rounds other values in their place, can miss the bound.
Values may be sent and summed in bfloat16 or wider, within the bound.
No kernel may reach another device: no remote copies, remote signals or barrier semaphores. Data moves between devices by JAX's collectives and lax.ppermute only.
A program may use at most 128 MiB of HBM per device.

```python
import jax
import jax.numpy as jnp
from jax import lax

D = 2048
CA = 1024
HEADS = 8
KW = 31
SEQ_LEN = 128
BLK = 64
NP = 4
PROWS = 128
PASS_DEV = 8
TOKENS = 2048
NB_DEV = 8
BLOCKS = 32
RQ = 32
MOST = 16
PASSAGES = 32
N_ST = 4
N_TP = 4


def request_table(key):
    hot_owner = jax.random.randint(jax.random.fold_in(key, 1), (), 0, N_ST)
    positions = jnp.arange(RQ)

    def one_device(device, dev_key):
        first_turn = (device - 1 - hot_owner) % N_ST - 1
        spread_turn = (first_turn + positions - MOST) % (N_ST - 1)
        owners_of = jnp.where(positions < MOST, hot_owner, (hot_owner + 1 + spread_turn) % N_ST)
        owners_of = owners_of[jax.random.permutation(dev_key, RQ)]
        local_index = jax.random.randint(jax.random.fold_in(dev_key, 3), (RQ,), 0, PASS_DEV)
        return (owners_of * PASS_DEV + local_index).reshape(NB_DEV, NP)
    dev_keys = jax.random.split(jax.random.fold_in(key, 2), N_ST)
    table = jax.vmap(one_device)(jnp.arange(N_ST), dev_keys)
    return table.reshape(BLOCKS, NP).astype(jnp.int32)


def store_rows(key):
    return jnp.clip(jax.random.normal(jax.random.fold_in(key, 12), (PASSAGES, PROWS, D), jnp.float32), -6.0, 6.0)


def draw_passage_ids(key, part):
    return request_table(jax.random.fold_in(key, 11))


def draw_store(key, part):
    return store_rows(key).astype(jnp.bfloat16)


def draw_tokens(key, part):
    plain_rows = jnp.clip(jax.random.normal(jax.random.fold_in(key, 13), (TOKENS, D), jnp.float32), -6.0, 6.0)
    return plain_rows.astype(jnp.bfloat16)


def draw_conv_taps(key, part):
    channel = jnp.arange(CA).astype(jnp.float32)
    channel_scale = jnp.exp(1.5 * (2.0 * channel / CA - 1.0)) * KW ** (-0.5)
    tap_draw = jnp.clip(jax.random.normal(jax.random.fold_in(key, 31), (KW, CA), jnp.float32), -6.0, 6.0)
    return jnp.clip(tap_draw * channel_scale, -5.0, 5.0).astype(jnp.bfloat16)


def draw_query_proj(key, part):
    fresh_draw = jax.random.normal(jax.random.fold_in(key, 22), (D, D), jnp.float32) * D ** (-0.5)
    return jnp.clip(fresh_draw, -1.0, 1.0).astype(jnp.bfloat16)


def draw_key_proj(key, part):
    fresh_draw = jax.random.normal(jax.random.fold_in(key, 23), (D, D), jnp.float32) * D ** (-0.5)
    return jnp.clip(fresh_draw, -1.0, 1.0).astype(jnp.bfloat16)


def shard_levels(stream_key, dims, pieces, smallest, high):
    gain, own = 1.0, jax.random.fold_in(stream_key, 6)
    for axis_at, blocks in pieces:
        steps = jnp.exp(jax.random.uniform(jax.random.fold_in(own, axis_at), (blocks,), jnp.float32, smallest / len(pieces), high / len(pieces)))
        gain = gain * jnp.repeat(steps, dims[axis_at] // blocks).reshape([-1 if axis == axis_at else 1 for axis in range(len(dims))])
    return gain


def normal_values(own_key, dims, scale, reach, cuts=(), dtype=jnp.bfloat16):
    drawn = jax.random.normal(own_key, dims, jnp.float32) * scale
    if len(cuts) > 0:
        drawn = shard_levels(own_key, dims, cuts, -0.22, 0.18) * drawn
    return jnp.clip(drawn, min=-reach, max=reach).astype(dtype)


def setup_inputs(seed: int = 0, part: int = 0) -> dict:
    streams_of = jax.random.split(jax.random.key(seed), 17)
    part_keys = jax.random.split(jax.random.fold_in(streams_of[16], part), 17)
    return {
        "tokens": draw_tokens(jax.random.fold_in(jax.random.fold_in(streams_of[16], part), 71), part),
        "store": draw_store(jax.random.fold_in(jax.random.fold_in(streams_of[16], part), 71), part),
        "passage_ids": draw_passage_ids(jax.random.fold_in(jax.random.fold_in(streams_of[16], part), 71), part),
        "mix_gain": jnp.clip(1.0 + 0.18 * jax.random.normal(streams_of[3], (D,), jnp.float32), 0.1, 1.9),
        "glu_value": normal_values(streams_of[4], (D, CA), D ** -0.5, 0.125, ((1, 4),)),
        "glu_gate": normal_values(streams_of[5], (D, CA), D ** -0.5, 0.125, ((1, 4),)),
        "conv_taps": draw_conv_taps(jax.random.fold_in(streams_of[16], 71), part),
        "channel_gain": jnp.clip(1.0 + 0.18 * jax.random.normal(streams_of[7], (CA,), jnp.float32), 0.1, 1.9),
        "mix_out": normal_values(streams_of[8], (CA, D), CA ** -0.5, 0.1875, ((0, 4),)),
        "query_gain": jnp.clip(1.0 + 0.18 * jax.random.normal(streams_of[9], (D,), jnp.float32), 0.1, 1.9),
        "passage_gain": jnp.clip(1.0 + 0.18 * jax.random.normal(streams_of[10], (D,), jnp.float32), 0.1, 1.9),
        "query_proj": draw_query_proj(jax.random.fold_in(streams_of[16], 71), part),
        "key_proj": draw_key_proj(jax.random.fold_in(streams_of[16], 71), part),
        "value_proj": normal_values(streams_of[13], (D, D), D ** -0.5, 0.125, ((1, 4),)),
        "attn_out": normal_values(streams_of[14], (D, D), D ** -0.5, 0.125, ((0, 4),)),
        "blend_gain": jnp.clip(jax.random.uniform(streams_of[15], (D,), jnp.float32, 0.5, 3.0), 0.5, 3.0),
    }


EPS = 1e-06

def rms_rows(row_data, gain_vec):
    floats = row_data.astype(jnp.float32)
    inv_scale = lax.rsqrt(lax.optimization_barrier(jnp.mean(floats * floats, axis=-1, keepdims=True)) + EPS)
    return (floats * inv_scale * gain_vec.astype(jnp.float32)).astype(jnp.bfloat16)

def depthwise(gated_rows, conv_taps):
    span_width = conv_taps.shape[0]
    half_span = (span_width - 1) // 2
    seq_length = gated_rows.shape[1]
    padded = jnp.pad(gated_rows.astype(jnp.float32), ((0, 0), (half_span, span_width - 1 - half_span), (0, 0)))
    running = jnp.zeros(gated_rows.shape, jnp.float32)
    for tap_index in range(span_width):
        running = running + padded[:, tap_index:tap_index + seq_length] * conv_taps[tap_index].astype(jnp.float32)
    return running

def passage_attention(queries, keys_values, head_count):
    groups, block_len, span_width = queries.shape
    head_dim = span_width // head_count
    row_count = keys_values.shape[1]
    query_heads = queries.astype(jnp.float32).reshape(groups, block_len, head_count, head_dim)
    key_heads = keys_values[:, :, :span_width].astype(jnp.float32).reshape(groups, row_count, head_count, head_dim)
    value_heads = keys_values[:, :, span_width:].astype(jnp.float32).reshape(groups, row_count, head_count, head_dim)
    scores = jnp.einsum('gqhd,grhd->ghqr', query_heads, key_heads) * head_dim ** (-0.5)
    row_top = lax.optimization_barrier(jnp.max(scores, axis=-1))
    exponent = jnp.exp(scores - row_top[..., None])
    row_sum = lax.optimization_barrier(jnp.sum(exponent, axis=-1))
    weights = exponent.astype(jnp.bfloat16).astype(jnp.float32)
    outputs = jnp.einsum('ghqr,grhd->gqhd', weights, value_heads).astype(jnp.bfloat16)
    return (outputs.reshape(groups, block_len, span_width), row_top, row_sum)

def combine(outs, tops, sums, head_count):
    batch_count, passage_count, block_len, span_width = outs.shape
    head_dim = span_width // head_count
    best_top = lax.optimization_barrier(jnp.max(tops, axis=1, keepdims=True))
    weight = jnp.exp(tops - best_top)
    numerator = jnp.einsum('bphq,bpqhd->bqhd', weight, outs.astype(jnp.float32).reshape(batch_count, passage_count, block_len, head_count, head_dim))
    denominator = lax.optimization_barrier(jnp.sum(weight * sums, axis=1))
    result = numerator / jnp.transpose(denominator, (0, 2, 1))[..., None]
    return result.reshape(batch_count, block_len, span_width).astype(jnp.bfloat16)

def reference(tokens, store, passage_ids, mix_gain, glu_value, glu_gate, conv_taps, channel_gain, mix_out, query_gain, passage_gain, query_proj, key_proj, value_proj, attn_out, blend_gain):
    mix_input = rms_rows(tokens, mix_gain)
    value_part = jnp.dot(mix_input, glu_value, preferred_element_type=jnp.float32)
    gate_part = jnp.dot(mix_input, glu_gate, preferred_element_type=jnp.float32)
    gated_rows = (value_part * jax.nn.sigmoid(gate_part)).astype(jnp.bfloat16)
    conv_rows = depthwise(gated_rows.reshape(-1, SEQ_LEN, CA), conv_taps).reshape(-1, CA)
    row_mean = lax.optimization_barrier(jnp.mean(conv_rows, axis=1, keepdims=True))
    row_var = lax.optimization_barrier(jnp.mean(conv_rows * conv_rows, axis=1, keepdims=True)) - row_mean * row_mean
    activation = jax.nn.silu((conv_rows - row_mean) * lax.rsqrt(row_var + EPS) * channel_gain.astype(jnp.float32)).astype(jnp.bfloat16)
    queries = jnp.dot(rms_rows(tokens, query_gain), query_proj, preferred_element_type=jnp.float32).astype(jnp.bfloat16)
    passage_rows = rms_rows(store.reshape(-1, D), passage_gain)
    key_rows = jnp.dot(passage_rows, key_proj, preferred_element_type=jnp.float32).astype(jnp.bfloat16)
    value_rows = jnp.dot(passage_rows, value_proj, preferred_element_type=jnp.float32).astype(jnp.bfloat16)
    memory = jnp.concatenate([key_rows, value_rows], axis=1).reshape(store.shape[0], store.shape[1], 2 * D)

    def one_block(inputs):
        block_queries, block_ids = inputs
        wanted = memory[block_ids]
        repeated = jnp.broadcast_to(block_queries[None], (NP, BLK, D))
        part_out, part_top, part_sum = passage_attention(repeated, wanted, HEADS)
        return combine(part_out[None], part_top[None], part_sum[None], HEADS)[0]
    attended = lax.map(one_block, (queries.reshape(-1, BLK, D), passage_ids)).reshape(-1, D)
    channel_group = CA // N_TP
    column_group = D // N_TP
    running = jnp.zeros((tokens.shape[0], D), jnp.float32)
    for shard_index in range(N_TP):
        conv_part = jnp.dot(activation[:, shard_index * channel_group:(shard_index + 1) * channel_group], mix_out[shard_index * channel_group:(shard_index + 1) * channel_group], preferred_element_type=jnp.float32)
        attn_part = jnp.dot(attended[:, shard_index * column_group:(shard_index + 1) * column_group], attn_out[shard_index * column_group:(shard_index + 1) * column_group], preferred_element_type=jnp.float32)
        partial_value = (conv_part + blend_gain.astype(jnp.float32) * attn_part).astype(jnp.bfloat16)
        partial_value = lax.optimization_barrier(partial_value)
        running = running + partial_value.astype(jnp.float32)
    return running.astype(jnp.bfloat16)
```

```python
import jax
import jax.numpy as jnp
from jax import lax
from jax.experimental import pallas as pl
from jax.experimental.pallas import tpu as pltpu
from jax.sharding import PartitionSpec as P

CA = 1024
HD = 256
SEQ_LEN = 128


EPS = 1e-06


def rms_rows(row_data, gain_vec):
    floats = row_data.astype(jnp.float32)
    inv_scale = lax.rsqrt(jnp.mean(floats * floats, axis=-1, keepdims=True) + EPS)
    return (floats * inv_scale * gain_vec).astype(jnp.bfloat16)


def depthwise(gated_rows, conv_taps):
    span_width = conv_taps.shape[0]
    half_span = (span_width - 1) // 2
    seq_length = gated_rows.shape[1]
    padded = jnp.pad(
        gated_rows.astype(jnp.float32), ((0, 0), (half_span, span_width - 1 - half_span), (0, 0))
    )
    running = jnp.zeros(gated_rows.shape, jnp.float32)
    for tap_index in range(span_width):
        running = running + padded[:, tap_index : tap_index + seq_length] * conv_taps[
            tap_index
        ].astype(jnp.float32)
    return running


NEVER = -1e30
BATCH = 4


def shifted(value, axis, step):
    size = lax.axis_size(axis)
    return lax.ppermute(value, axis, [(i, (i + step) % size) for i in range(size)])


def owner_attention(me, ids, query_list, keys, values, block_len, per_block, pass_rows):
    sources = len(query_list)
    rows, head_width = query_list[0].shape
    blocks = rows // block_len
    heads = head_width // HD
    held = keys.shape[0] // pass_rows
    slots = blocks * per_block + BATCH
    scale = HD ** (-0.5)
    pair = 128 // block_len

    def kernel(me_ref, ids_ref, *refs):
        query_refs = refs[:sources]
        key_ref, value_ref = refs[sources : sources + 2]
        out_refs = refs[sources + 2 : 2 * sources + 2]
        stat_refs = refs[2 * sources + 2 : 3 * sources + 2]
        list_block, list_pass, part_ref, top_ref, sum_ref = refs[3 * sources + 2 :]
        first = me_ref[0] * held
        lane = lax.broadcasted_iota(jnp.int32, (block_len, 128), 1)
        for source in range(sources):
            count = jnp.int32(0)
            starts = []
            for block in range(blocks):
                starts.append(count)
                for j in range(per_block):
                    where = ids_ref[source, block * per_block + j] - first
                    list_block[count] = jnp.int32(block)
                    list_pass[count] = jnp.clip(where, 0, held - 1)
                    mine = jnp.logical_and(where >= 0, where < held)
                    count = count + mine.astype(jnp.int32)
            starts.append(count)
            for u in range(BATCH):
                list_block[count + u] = jnp.int32(0)
                list_pass[count + u] = jnp.int32(0)
            trips = jnp.maximum((count + BATCH - 1) // BATCH, 1)
            query_ref = query_refs[source]

            def batch(i, carry):
                for u in range(BATCH):
                    slot = i * BATCH + u
                    block_at = pl.multiple_of(list_block[slot] * block_len, block_len)
                    pass_at = pl.multiple_of(list_pass[slot] * pass_rows, pass_rows)
                    for h in range(heads):
                        cols = slice(h * HD, (h + 1) * HD)
                        q = query_ref[pl.ds(block_at, block_len), cols]
                        k = key_ref[pl.ds(pass_at, pass_rows), cols]
                        v = value_ref[pl.ds(pass_at, pass_rows), cols]
                        scores = lax.dot_general(
                            q, k, (((1,), (1,)), ((), ())), preferred_element_type=jnp.float32
                        ) * scale
                        top = jnp.max(scores, axis=1, keepdims=True)
                        exponent = jnp.exp(scores - top)
                        total = jnp.sum(exponent, axis=1, keepdims=True)
                        out = jnp.dot(
                            exponent.astype(jnp.bfloat16), v, preferred_element_type=jnp.float32
                        )
                        part_ref[slot, :, cols] = out.astype(jnp.bfloat16)
                        top_ref[slot, h] = jnp.broadcast_to(top, (block_len, 128))
                        sum_ref[slot, h] = jnp.broadcast_to(total, (block_len, 128))
                return carry

            lax.fori_loop(0, trips, batch, 0)
            tiles = []
            for block in range(blocks):
                held_here = starts[block + 1] - starts[block]
                at = [
                    jnp.where(j < held_here, starts[block] + j, 0) for j in range(per_block)
                ]
                tile = jnp.zeros((block_len, 128), jnp.float32)
                for h in range(heads):
                    cols = slice(h * HD, (h + 1) * HD)
                    tops = [
                        jnp.where(j < held_here, top_ref[at[j], h], NEVER)
                        for j in range(per_block)
                    ]
                    best = tops[0]
                    for j in range(1, per_block):
                        best = jnp.maximum(best, tops[j])
                    total = jnp.zeros((block_len, 128), jnp.float32)
                    merged = jnp.zeros((block_len, HD), jnp.float32)
                    for j in range(per_block):
                        weight = jnp.where(j < held_here, jnp.exp(tops[j] - best), 0.0)
                        total = total + weight * sum_ref[at[j], h]
                        wide = jnp.concatenate([weight] * (HD // 128), axis=1)
                        merged = merged + wide * part_ref[at[j], :, cols].astype(jnp.float32)
                    out_refs[source][block * block_len : (block + 1) * block_len, cols] = (
                        merged.astype(jnp.bfloat16)
                    )
                    tile = jnp.where(lane == h, best, tile)
                    tile = jnp.where(lane == heads + h, total, tile)
                tiles.append(tile)
            for at_pair in range(0, blocks, pair):
                square = jnp.concatenate(tiles[at_pair : at_pair + pair], axis=0)
                stat_refs[source][:, at_pair * block_len : (at_pair + pair) * block_len] = (
                    square.T[:8]
                )

    whole = pl.BlockSpec(memory_space=pltpu.VMEM)
    scalar = pl.BlockSpec(memory_space=pltpu.SMEM)
    outs = pl.pallas_call(
        kernel,
        out_shape=[jax.ShapeDtypeStruct((rows, head_width), jnp.bfloat16)] * sources
        + [jax.ShapeDtypeStruct((8, rows), jnp.float32)] * sources,
        in_specs=[scalar, scalar] + [whole] * (sources + 2),
        out_specs=[whole] * (2 * sources),
        scratch_shapes=[
            pltpu.SMEM((slots,), jnp.int32),
            pltpu.SMEM((slots,), jnp.int32),
            pltpu.VMEM((slots, block_len, head_width), jnp.bfloat16),
            pltpu.VMEM((slots, heads, block_len, 128), jnp.float32),
            pltpu.VMEM((slots, heads, block_len, 128), jnp.float32),
        ],
        name="owner_attention",
    )(me, ids, *query_list, keys, values)
    return outs[:sources], outs[sources:]


def merge_owners(out_list, stat_list):
    sources = len(out_list)
    rows, head_width = out_list[0].shape
    heads = head_width // HD

    def kernel(*refs):
        out_refs = refs[:sources]
        stat_refs = refs[sources : 2 * sources]
        result_ref = refs[2 * sources]
        for at in range(0, rows, 128):
            stats = [ref[:, at : at + 128] for ref in stat_refs]
            best = [stats[0][h : h + 1] for h in range(heads)]
            for s in range(1, sources):
                best = [jnp.maximum(best[h], stats[s][h : h + 1]) for h in range(heads)]
            weights = [
                [jnp.exp(stats[s][h : h + 1] - best[h]) for h in range(heads)]
                for s in range(sources)
            ]
            for h in range(heads):
                total = weights[0][h] * stats[0][heads + h : heads + h + 1]
                for s in range(1, sources):
                    total = total + weights[s][h] * stats[s][heads + h : heads + h + 1]
                table = jnp.concatenate(
                    [weights[s][h] / total for s in range(sources)]
                    + [jnp.zeros((128 - sources, 128), jnp.float32)],
                    axis=0,
                ).T
                cols = slice(h * HD, (h + 1) * HD)
                merged = jnp.zeros((128, HD), jnp.float32)
                for s in range(sources):
                    merged = merged + table[:, s : s + 1] * out_refs[s][
                        at : at + 128, cols
                    ].astype(jnp.float32)
                result_ref[at : at + 128, cols] = merged.astype(jnp.bfloat16)

    whole = pl.BlockSpec(memory_space=pltpu.VMEM)
    return pl.pallas_call(
        kernel,
        out_shape=jax.ShapeDtypeStruct((rows, head_width), jnp.bfloat16),
        in_specs=[whole] * (2 * sources),
        out_specs=whole,
        name="merge_owners",
    )(*out_list, *stat_list)


def local(
    tokens,
    store,
    passage_ids,
    mix_gain,
    glu_value,
    glu_gate,
    conv_taps,
    channel_gain,
    mix_out,
    query_gain,
    passage_gain,
    query_proj,
    key_proj,
    value_proj,
    attn_out,
    blend_gain,
):
    owners = lax.axis_size("st")
    shards = lax.axis_size("tp")
    me = lax.axis_index("st").astype(jnp.int32)
    mine = lax.axis_index("tp")
    tok_rows, model_width = tokens.shape
    local_channels = glu_value.shape[1]
    head_width = query_proj.shape[1]
    block_count, per_block = passage_ids.shape
    block_len = tok_rows // block_count
    pass_local, pass_rows, _ = store.shape
    blocks_per_shard = block_count // shards
    chunks = CHUNKS if blocks_per_shard % CHUNKS == 0 else 1
    run = blocks_per_shard // chunks * block_len
    steps = range(1, owners)

    def cut(rows, c):
        return rows.reshape(shards, chunks, run, -1)[:, c].reshape(shards * run, -1)

    queries = jnp.dot(
        rms_rows(tokens, query_gain), query_proj, preferred_element_type=jnp.float32
    ).astype(jnp.bfloat16)
    id_list = [passage_ids] + [shifted(passage_ids, "st", k) for k in steps]
    all_ids = jnp.stack(id_list)
    query_chunks = []
    for c in range(chunks):
        own = cut(queries, c)
        query_chunks.append([own] + [shifted(own, "st", k) for k in steps])
    normed_store = rms_rows(store.reshape(pass_local * pass_rows, model_width), passage_gain)
    key_rows = jnp.dot(normed_store, key_proj, preferred_element_type=jnp.float32).astype(
        jnp.bfloat16
    )
    value_rows = jnp.dot(normed_store, value_proj, preferred_element_type=jnp.float32).astype(
        jnp.bfloat16
    )
    mix_input = rms_rows(tokens, mix_gain)
    value_part = jnp.dot(mix_input, glu_value, preferred_element_type=jnp.float32)
    gate_part = jnp.dot(mix_input, glu_gate, preferred_element_type=jnp.float32)
    gated_rows = (value_part * jax.nn.sigmoid(gate_part)).astype(jnp.bfloat16)
    conv_rows = depthwise(gated_rows.reshape(-1, SEQ_LEN, local_channels), conv_taps).reshape(
        tok_rows, local_channels
    )
    sums = jnp.stack([jnp.sum(conv_rows, axis=1), jnp.sum(conv_rows * conv_rows, axis=1)])
    channel_total = sums
    for k in range(1, shards):
        channel_total = channel_total + shifted(sums, "tp", k)
    answers = []
    for c in range(chunks):
        ids = all_ids.reshape(
            owners, shards, chunks, blocks_per_shard // chunks * per_block
        )[:, :, c].reshape(owners, -1)
        out_list, stat_list = owner_attention(
            me[None], ids, query_chunks[c], key_rows, value_rows, block_len, per_block, pass_rows
        )
        answers.append(
            (
                [out_list[0]] + [shifted(out_list[k], "st", -k) for k in steps],
                [stat_list[0]] + [shifted(stat_list[k], "st", -k) for k in steps],
            )
        )
    row_mean = channel_total[0] / CA
    row_var = channel_total[1] / CA - row_mean * row_mean
    activation = jax.nn.silu(
        (conv_rows - row_mean[:, None]) * lax.rsqrt(row_var + EPS)[:, None] * channel_gain
    ).astype(jnp.bfloat16)
    results = []
    for c in range(chunks):
        attended = merge_owners(*answers[c])
        conv_term = jnp.dot(cut(activation, c), mix_out, preferred_element_type=jnp.float32)
        attn_term = jnp.dot(attended, attn_out, preferred_element_type=jnp.float32)
        partial = (
            (conv_term + blend_gain * attn_term).astype(jnp.bfloat16).reshape(shards, run, -1)
        )
        order = sorted(range(1, shards), key=lambda k: -min(k, shards - k))
        pieces = [
            shifted(
                lax.dynamic_index_in_dim(partial, (mine + k) % shards, 0, keepdims=False),
                "tp",
                k,
            )
            for k in order
        ]
        total = lax.dynamic_index_in_dim(partial, mine, 0, keepdims=False).astype(jnp.float32)
        for piece in pieces:
            total = total + piece.astype(jnp.float32)
        results.append(total.astype(jnp.bfloat16))
    return jnp.concatenate(results, axis=0)


CHUNKS = 2


def solution(mesh):
    in_specs = (
        P(("grp", "st"), None),
        P(("grp", "st"), None, None),
        P(("grp", "st"), None),
        P(),
        P(None, "tp"),
        P(None, "tp"),
        P(None, "tp"),
        P("tp"),
        P("tp", None),
        P(),
        P(),
        P(None, "tp"),
        P(None, "tp"),
        P(None, "tp"),
        P("tp", None),
        P(),
    )
    out_specs = P(("grp", "st", "tp"), None)
    return jax.shard_map(local, mesh=mesh, in_specs=in_specs, out_specs=out_specs, check_vma=False)
```

```python
import jax
import jax.numpy as jnp
from jax import lax
from jax.experimental import pallas as pl
from jax.experimental.pallas import tpu as pltpu
from jax.sharding import PartitionSpec as P

CA = 1024
HD = 256
SEQ_LEN = 128


EPS = 1e-06


def rms_rows(row_data, gain_vec):
    floats = row_data.astype(jnp.float32)
    inv_scale = lax.rsqrt(jnp.mean(floats * floats, axis=-1, keepdims=True) + EPS)
    return (floats * inv_scale * gain_vec).astype(jnp.bfloat16)


def depthwise(gated_rows, conv_taps):
    span_width = conv_taps.shape[0]
    half_span = (span_width - 1) // 2
    seq_length = gated_rows.shape[1]
    padded = jnp.pad(
        gated_rows.astype(jnp.float32), ((0, 0), (half_span, span_width - 1 - half_span), (0, 0))
    )
    running = jnp.zeros(gated_rows.shape, jnp.float32)
    for tap_index in range(span_width):
        running = running + padded[:, tap_index : tap_index + seq_length] * conv_taps[
            tap_index
        ].astype(jnp.float32)
    return running


NEVER = -1e30
BATCH = 4


def shifted(value, axis, step):
    size = lax.axis_size(axis)
    return lax.ppermute(value, axis, [(i, (i + step) % size) for i in range(size)])


def passage_planes(store_rows, gain_vec, key_proj, value_proj):
    total_rows, model_width = store_rows.shape
    planes = key_proj.shape[1] // 128
    step_rows = min(256, total_rows)

    def kernel(row_ref, gain_ref, key_w, value_w, key_ref, value_ref):
        floats = row_ref[...].astype(jnp.float32)
        inv_scale = lax.rsqrt(jnp.mean(floats * floats, axis=-1, keepdims=True) + EPS)
        normed = (floats * inv_scale * gain_ref[...]).astype(jnp.bfloat16)
        for weight, target in ((key_w, key_ref), (value_w, value_ref)):
            result = jnp.dot(normed, weight[...], preferred_element_type=jnp.float32)
            for c in range(planes):
                target[c] = result[:, c * 128 : (c + 1) * 128].astype(jnp.bfloat16)

    whole = pl.BlockSpec(memory_space=pltpu.VMEM)
    plane_spec = pl.BlockSpec((planes, step_rows, 128), lambda i: (0, i, 0))
    return pl.pallas_call(
        kernel,
        grid=(total_rows // step_rows,),
        out_shape=[jax.ShapeDtypeStruct((planes, total_rows, 128), jnp.bfloat16)] * 2,
        in_specs=[pl.BlockSpec((step_rows, model_width), lambda i: (i, 0)), whole, whole, whole],
        out_specs=[plane_spec, plane_spec],
        name="passage_planes",
    )(store_rows, gain_vec[None], key_proj, value_proj)


def stat_place(rows, head_width):
    across = head_width // 128
    tiles = 3 * (rows // 128)
    places = [(rows + 8 * (t // across), 128 * (t % across)) for t in range(tiles)]
    return places, 16 * -(-(-(-tiles // across)) // 2)


def owner_attention(me, ids, query_list, keys, values, block_len, per_block, pass_rows):
    sources = len(query_list)
    head_width = query_list[0].shape[1]
    blocks = ids.shape[1] // per_block
    rows = blocks * block_len
    heads = head_width // HD
    held = keys.shape[1] // pass_rows
    lanes = HD // 128
    places, extra = stat_place(rows, head_width)
    slots = blocks * per_block + BATCH
    scale = HD ** (-0.5)
    pair = 128 // block_len

    def kernel(me_ref, ids_ref, *refs):
        query_refs = refs[:sources]
        key_ref, value_ref = refs[sources : sources + 2]
        out_refs = refs[sources + 2 : 2 * sources + 2]
        list_block, list_pass, part_ref, top_ref, sum_ref = refs[2 * sources + 2 :]
        first = me_ref[0] * held
        lane = lax.broadcasted_iota(jnp.int32, (block_len, 128), 1)
        for source in range(sources):
            count = jnp.int32(0)
            starts = []
            for block in range(blocks):
                starts.append(count)
                for j in range(per_block):
                    where = ids_ref[source, block * per_block + j] - first
                    list_block[count] = jnp.int32(block)
                    list_pass[count] = jnp.clip(where, 0, held - 1)
                    mine = jnp.logical_and(where >= 0, where < held)
                    count = count + mine.astype(jnp.int32)
            starts.append(count)
            for u in range(BATCH):
                list_block[count + u] = jnp.int32(0)
                list_pass[count + u] = jnp.int32(0)
            trips = jnp.maximum((count + BATCH - 1) // BATCH, 1)
            query_ref = query_refs[source]

            def batch(i, carry):
                for u in range(BATCH):
                    slot = i * BATCH + u
                    block_at = pl.multiple_of(list_block[slot] * block_len, block_len)
                    pass_at = pl.multiple_of(list_pass[slot] * pass_rows, pass_rows)
                    for h in range(heads):
                        cols = slice(h * HD, (h + 1) * HD)
                        q = query_ref[pl.ds(block_at, block_len), cols]
                        k, v = (
                            jnp.concatenate(
                                [
                                    ref[h * lanes + c, pl.ds(pass_at, pass_rows), :]
                                    for c in range(lanes)
                                ],
                                axis=1,
                            )
                            for ref in (key_ref, value_ref)
                        )
                        scores = lax.dot_general(
                            q, k, (((1,), (1,)), ((), ())), preferred_element_type=jnp.float32
                        ) * scale
                        top = jnp.max(scores, axis=1, keepdims=True)
                        exponent = jnp.exp(scores - top)
                        total = jnp.sum(exponent, axis=1, keepdims=True)
                        out = jnp.dot(
                            exponent.astype(jnp.bfloat16), v, preferred_element_type=jnp.float32
                        )
                        for c in range(lanes):
                            part_ref[slot, h * lanes + c] = out[
                                :, c * 128 : (c + 1) * 128
                            ].astype(jnp.bfloat16)
                        top_ref[slot, h] = jnp.broadcast_to(top, (block_len, 128))
                        sum_ref[slot, h] = jnp.broadcast_to(total, (block_len, 128))
                return carry

            lax.fori_loop(0, trips, batch, 0)
            tiles = []
            for block in range(blocks):
                held_here = starts[block + 1] - starts[block]
                at = [
                    jnp.where(j < held_here, starts[block] + j, 0) for j in range(per_block)
                ]
                tile = jnp.zeros((block_len, 128), jnp.float32)
                for h in range(heads):
                    cols = slice(h * HD, (h + 1) * HD)
                    tops = [
                        jnp.where(j < held_here, top_ref[at[j], h], NEVER)
                        for j in range(per_block)
                    ]
                    best = tops[0]
                    for j in range(1, per_block):
                        best = jnp.maximum(best, tops[j])
                    total = jnp.zeros((block_len, 128), jnp.float32)
                    merged = [jnp.zeros((block_len, 128), jnp.float32)] * lanes
                    for j in range(per_block):
                        weight = jnp.where(j < held_here, jnp.exp(tops[j] - best), 0.0)
                        total = total + weight * sum_ref[at[j], h]
                        merged = [
                            merged[c]
                            + weight * part_ref[at[j], h * lanes + c].astype(jnp.float32)
                            for c in range(lanes)
                        ]
                    out_refs[source][block * block_len : (block + 1) * block_len, cols] = (
                        jnp.concatenate(merged, axis=1).astype(jnp.bfloat16)
                    )
                    tile = jnp.where(lane == h, best, tile)
                    tile = jnp.where(lane == heads + h, total, tile)
                tiles.append(tile)
            for at_pair in range(0, blocks, pair):
                rest = jnp.concatenate(tiles[at_pair : at_pair + pair], axis=0).T[:8]
                for piece in range(3):
                    row, col = places[piece * (rows // 128) + at_pair // pair]
                    rounded = rest.astype(jnp.bfloat16)
                    out_refs[source][row : row + 8, col : col + 128] = rounded
                    rest = rest - rounded.astype(jnp.float32)

    whole = pl.BlockSpec(memory_space=pltpu.VMEM)
    scalar = pl.BlockSpec(memory_space=pltpu.SMEM)
    outs = pl.pallas_call(
        kernel,
        out_shape=[jax.ShapeDtypeStruct((rows + extra, head_width), jnp.bfloat16)] * sources,
        in_specs=[scalar, scalar] + [whole] * (sources + 2),
        out_specs=[whole] * sources,
        scratch_shapes=[
            pltpu.SMEM((slots,), jnp.int32),
            pltpu.SMEM((slots,), jnp.int32),
            pltpu.VMEM((slots, head_width // 128, block_len, 128), jnp.bfloat16),
            pltpu.VMEM((slots, heads, block_len, 128), jnp.float32),
            pltpu.VMEM((slots, heads, block_len, 128), jnp.float32),
        ],
        name="owner_attention",
    )(me, ids, *query_list, keys, values)
    return outs


def merge_owners(out_list, rows):
    sources = len(out_list)
    head_width = out_list[0].shape[1]
    heads = head_width // HD
    places, _ = stat_place(rows, head_width)

    def kernel(*refs):
        out_refs = refs[:sources]
        result_ref = refs[sources]
        for at in range(0, rows, 128):
            stats = []
            for ref in out_refs:
                pieces = []
                for piece in range(3):
                    row, col = places[piece * (rows // 128) + at // 128]
                    pieces.append(ref[row : row + 8, col : col + 128].astype(jnp.float32))
                stats.append(pieces[2] + pieces[1] + pieces[0])
            best = [stats[0][h : h + 1] for h in range(heads)]
            for s in range(1, sources):
                best = [jnp.maximum(best[h], stats[s][h : h + 1]) for h in range(heads)]
            weights = [
                [jnp.exp(stats[s][h : h + 1] - best[h]) for h in range(heads)]
                for s in range(sources)
            ]
            for h in range(heads):
                total = weights[0][h] * stats[0][heads + h : heads + h + 1]
                for s in range(1, sources):
                    total = total + weights[s][h] * stats[s][heads + h : heads + h + 1]
                table = jnp.concatenate(
                    [weights[s][h] / total for s in range(sources)]
                    + [jnp.zeros((128 - sources, 128), jnp.float32)],
                    axis=0,
                ).T
                cols = slice(h * HD, (h + 1) * HD)
                merged = jnp.zeros((128, HD), jnp.float32)
                for s in range(sources):
                    merged = merged + table[:, s : s + 1] * out_refs[s][
                        at : at + 128, cols
                    ].astype(jnp.float32)
                result_ref[at : at + 128, cols] = merged.astype(jnp.bfloat16)

    whole = pl.BlockSpec(memory_space=pltpu.VMEM)
    return pl.pallas_call(
        kernel,
        out_shape=jax.ShapeDtypeStruct((rows, head_width), jnp.bfloat16),
        in_specs=[whole] * sources,
        out_specs=whole,
        name="merge_owners",
    )(*out_list)


def local(
    tokens,
    store,
    passage_ids,
    mix_gain,
    glu_value,
    glu_gate,
    conv_taps,
    channel_gain,
    mix_out,
    query_gain,
    passage_gain,
    query_proj,
    key_proj,
    value_proj,
    attn_out,
    blend_gain,
):
    owners = lax.axis_size("st")
    shards = lax.axis_size("tp")
    me = lax.axis_index("st").astype(jnp.int32)
    mine = lax.axis_index("tp")
    tok_rows, model_width = tokens.shape
    local_channels = glu_value.shape[1]
    head_width = query_proj.shape[1]
    block_count, per_block = passage_ids.shape
    block_len = tok_rows // block_count
    pass_local, pass_rows, _ = store.shape
    blocks_per_shard = block_count // shards
    chunks = CHUNKS if blocks_per_shard % CHUNKS == 0 else 1
    run = blocks_per_shard // chunks * block_len
    steps = range(1, owners)

    def cut(rows, c):
        return rows.reshape(shards, chunks, run, -1)[:, c].reshape(shards * run, -1)

    queries = jnp.dot(
        rms_rows(tokens, query_gain), query_proj, preferred_element_type=jnp.float32
    ).astype(jnp.bfloat16)
    assert owners * pass_local <= 256
    query_chunks = []
    id_chunks = []
    for c in range(chunks):
        ids = passage_ids.reshape(shards, chunks, -1)[:, c].reshape(1, -1)
        id_rows = jnp.pad(
            ids.astype(jnp.bfloat16), ((0, 15), (0, head_width - ids.shape[1]))
        )
        own = jnp.concatenate([cut(queries, c), id_rows], axis=0)
        query_list = [own] + [shifted(own, "st", k) for k in steps]
        query_chunks.append(query_list)
        id_chunks.append(
            jnp.stack([q[shards * run, : ids.shape[1]] for q in query_list]).astype(jnp.int32)
        )
    key_planes, value_planes = passage_planes(
        store.reshape(pass_local * pass_rows, model_width), passage_gain, key_proj, value_proj
    )
    mix_input = rms_rows(tokens, mix_gain)
    value_part = jnp.dot(mix_input, glu_value, preferred_element_type=jnp.float32)
    gate_part = jnp.dot(mix_input, glu_gate, preferred_element_type=jnp.float32)
    gated_rows = (value_part * jax.nn.sigmoid(gate_part)).astype(jnp.bfloat16)
    conv_rows = depthwise(gated_rows.reshape(-1, SEQ_LEN, local_channels), conv_taps).reshape(
        tok_rows, local_channels
    )
    sums = jnp.stack([jnp.sum(conv_rows, axis=1), jnp.sum(conv_rows * conv_rows, axis=1)])
    channel_total = sums
    for k in range(1, shards):
        channel_total = channel_total + shifted(sums, "tp", k)
    answers = []
    for c in range(chunks):
        out_list = owner_attention(
            me[None],
            id_chunks[c],
            query_chunks[c],
            key_planes,
            value_planes,
            block_len,
            per_block,
            pass_rows,
        )
        answers.append([out_list[0]] + [shifted(out_list[k], "st", -k) for k in steps])
    row_mean = channel_total[0] / CA
    row_var = channel_total[1] / CA - row_mean * row_mean
    activation = jax.nn.silu(
        (conv_rows - row_mean[:, None]) * lax.rsqrt(row_var + EPS)[:, None] * channel_gain
    ).astype(jnp.bfloat16)
    results = []
    for c in range(chunks):
        attended = merge_owners(answers[c], shards * run)
        conv_term = jnp.dot(cut(activation, c), mix_out, preferred_element_type=jnp.float32)
        attn_term = jnp.dot(attended, attn_out, preferred_element_type=jnp.float32)
        partial = (
            (conv_term + blend_gain * attn_term).astype(jnp.bfloat16).reshape(shards, run, -1)
        )
        order = sorted(range(1, shards), key=lambda k: -min(k, shards - k))
        pieces = [
            shifted(
                lax.dynamic_index_in_dim(partial, (mine + k) % shards, 0, keepdims=False),
                "tp",
                k,
            )
            for k in order
        ]
        total = lax.dynamic_index_in_dim(partial, mine, 0, keepdims=False).astype(jnp.float32)
        for piece in pieces:
            total = total + piece.astype(jnp.float32)
        results.append(total.astype(jnp.bfloat16))
    return jnp.concatenate(results, axis=0)


CHUNKS = 2


def solution(mesh):
    in_specs = (
        P(("grp", "st"), None),
        P(("grp", "st"), None, None),
        P(("grp", "st"), None),
        P(),
        P(None, "tp"),
        P(None, "tp"),
        P(None, "tp"),
        P("tp"),
        P("tp", None),
        P(),
        P(),
        P(None, "tp"),
        P(None, "tp"),
        P(None, "tp"),
        P("tp", None),
        P(),
    )
    out_specs = P(("grp", "st", "tp"), None)
    return jax.shard_map(local, mesh=mesh, in_specs=in_specs, out_specs=out_specs, check_vma=False)
```

```python
import jax
import jax.numpy as jnp
from jax import lax
from jax.experimental import pallas as pl
from jax.experimental.pallas import tpu as pltpu
from jax.sharding import PartitionSpec as P

CA = 1024
HD = 256
SEQ_LEN = 128


EPS = 1e-06


def rms_rows(row_data, gain_vec):
    floats = row_data.astype(jnp.float32)
    inv_scale = lax.rsqrt(jnp.mean(floats * floats, axis=-1, keepdims=True) + EPS)
    return (floats * inv_scale * gain_vec).astype(jnp.bfloat16)


def depthwise(gated_rows, conv_taps):
    span_width = conv_taps.shape[0]
    half_span = (span_width - 1) // 2
    seq_length = gated_rows.shape[1]
    padded = jnp.pad(
        gated_rows.astype(jnp.float32), ((0, 0), (half_span, span_width - 1 - half_span), (0, 0))
    )
    running = jnp.zeros(gated_rows.shape, jnp.float32)
    for tap_index in range(span_width):
        running = running + padded[:, tap_index : tap_index + seq_length] * conv_taps[
            tap_index
        ].astype(jnp.float32)
    return running


NEVER = -1e30
BATCH = 4


def shifted(value, axis, step):
    size = lax.axis_size(axis)
    return lax.ppermute(value, axis, [(i, (i + step) % size) for i in range(size)])


def passage_planes(store_rows, gain_vec, key_proj, value_proj):
    total_rows, model_width = store_rows.shape
    planes = key_proj.shape[1] // 128
    step_rows = min(256, total_rows)

    def kernel(row_ref, gain_ref, key_w, value_w, key_ref, value_ref):
        floats = row_ref[...].astype(jnp.float32)
        inv_scale = lax.rsqrt(jnp.mean(floats * floats, axis=-1, keepdims=True) + EPS)
        normed = (floats * inv_scale * gain_ref[...]).astype(jnp.bfloat16)
        for weight, target in ((key_w, key_ref), (value_w, value_ref)):
            result = jnp.dot(normed, weight[...], preferred_element_type=jnp.float32)
            for c in range(planes):
                target[c] = result[:, c * 128 : (c + 1) * 128].astype(jnp.bfloat16)

    whole = pl.BlockSpec(memory_space=pltpu.VMEM)
    plane_spec = pl.BlockSpec((planes, step_rows, 128), lambda i: (0, i, 0))
    return pl.pallas_call(
        kernel,
        grid=(total_rows // step_rows,),
        out_shape=[jax.ShapeDtypeStruct((planes, total_rows, 128), jnp.bfloat16)] * 2,
        in_specs=[pl.BlockSpec((step_rows, model_width), lambda i: (i, 0)), whole, whole, whole],
        out_specs=[plane_spec, plane_spec],
        name="passage_planes",
    )(store_rows, gain_vec[None], key_proj, value_proj)


def stat_place(rows, head_width):
    across = head_width // 128
    tiles = 3 * (rows // 128)
    places = [(rows + 8 * (t // across), 128 * (t % across)) for t in range(tiles)]
    return places, 16 * -(-(-(-tiles // across)) // 2)


def owner_attention(me, ids, query_list, keys, values, block_len, per_block, pass_rows):
    sources = len(query_list)
    head_width = query_list[0].shape[1]
    blocks = ids.shape[1] // per_block
    rows = blocks * block_len
    heads = head_width // HD
    held = keys.shape[1] // pass_rows
    lanes = HD // 128
    places, extra = stat_place(rows, head_width)
    slots = blocks * per_block + BATCH
    scale = HD ** (-0.5)
    pair = 128 // block_len

    def kernel(me_ref, ids_ref, *refs):
        query_refs = refs[:sources]
        key_ref, value_ref = refs[sources : sources + 2]
        out_refs = refs[sources + 2 : 2 * sources + 2]
        list_block, list_pass, part_ref, top_ref, sum_ref, weight_ref = refs[2 * sources + 2 :]

        def held_rows(ref, h, at):
            return jnp.concatenate(
                [ref[h * lanes + c, pl.ds(at, pass_rows), :] for c in range(lanes)], axis=1
            )

        first = me_ref[0] * held
        lane = lax.broadcasted_iota(jnp.int32, (block_len, 128), 1)
        for source in range(sources):
            count = jnp.int32(0)
            starts = []
            for block in range(blocks):
                starts.append(count)
                for j in range(per_block):
                    where = ids_ref[source, block * per_block + j] - first
                    list_block[count] = jnp.int32(block)
                    list_pass[count] = jnp.clip(where, 0, held - 1)
                    mine = jnp.logical_and(where >= 0, where < held)
                    count = count + mine.astype(jnp.int32)
            starts.append(count)
            for u in range(BATCH):
                list_block[count + u] = jnp.int32(0)
                list_pass[count + u] = jnp.int32(0)
            trips = jnp.maximum((count + BATCH - 1) // BATCH, 1)
            query_ref = query_refs[source]

            def batch(i, carry):
                for u in range(BATCH):
                    slot = i * BATCH + u
                    block_at = pl.multiple_of(list_block[slot] * block_len, block_len)
                    pass_at = pl.multiple_of(list_pass[slot] * pass_rows, pass_rows)
                    for h in range(heads):
                        cols = slice(h * HD, (h + 1) * HD)
                        q = query_ref[pl.ds(block_at, block_len), cols]
                        k = held_rows(key_ref, h, pass_at)
                        scores = lax.dot_general(
                            q, k, (((1,), (1,)), ((), ())), preferred_element_type=jnp.float32
                        ) * scale
                        top = jnp.max(scores, axis=1, keepdims=True)
                        exponent = jnp.exp(scores - top)
                        total = jnp.sum(exponent, axis=1, keepdims=True)
                        weight_ref[slot, h] = exponent.astype(jnp.bfloat16)
                        top_ref[slot, h] = jnp.broadcast_to(top, (block_len, 128))
                        sum_ref[slot, h] = jnp.broadcast_to(total, (block_len, 128))
                return carry

            def weigh(i, carry):
                for u in range(BATCH):
                    slot = i * BATCH + u
                    pass_at = pl.multiple_of(list_pass[slot] * pass_rows, pass_rows)
                    for h in range(heads):
                        out = jnp.dot(
                            weight_ref[slot, h],
                            held_rows(value_ref, h, pass_at),
                            preferred_element_type=jnp.float32,
                        )
                        for c in range(lanes):
                            part_ref[slot, h * lanes + c] = out[
                                :, c * 128 : (c + 1) * 128
                            ].astype(jnp.bfloat16)
                return carry

            lax.fori_loop(0, trips, batch, 0)
            lax.fori_loop(0, trips, weigh, 0)
            tiles = []
            for block in range(blocks):
                held_here = starts[block + 1] - starts[block]
                at = [
                    jnp.where(j < held_here, starts[block] + j, 0) for j in range(per_block)
                ]
                tile = jnp.zeros((block_len, 128), jnp.float32)
                for h in range(heads):
                    cols = slice(h * HD, (h + 1) * HD)
                    tops = [
                        jnp.where(j < held_here, top_ref[at[j], h], NEVER)
                        for j in range(per_block)
                    ]
                    best = tops[0]
                    for j in range(1, per_block):
                        best = jnp.maximum(best, tops[j])
                    total = jnp.zeros((block_len, 128), jnp.float32)
                    merged = [jnp.zeros((block_len, 128), jnp.float32)] * lanes
                    for j in range(per_block):
                        weight = jnp.where(j < held_here, jnp.exp(tops[j] - best), 0.0)
                        total = total + weight * sum_ref[at[j], h]
                        merged = [
                            merged[c]
                            + weight * part_ref[at[j], h * lanes + c].astype(jnp.float32)
                            for c in range(lanes)
                        ]
                    out_refs[source][block * block_len : (block + 1) * block_len, cols] = (
                        jnp.concatenate(merged, axis=1).astype(jnp.bfloat16)
                    )
                    tile = jnp.where(lane == h, best, tile)
                    tile = jnp.where(lane == heads + h, total, tile)
                tiles.append(tile)
            for at_pair in range(0, blocks, pair):
                rest = jnp.concatenate(tiles[at_pair : at_pair + pair], axis=0).T[:8]
                for piece in range(3):
                    row, col = places[piece * (rows // 128) + at_pair // pair]
                    rounded = rest.astype(jnp.bfloat16)
                    out_refs[source][row : row + 8, col : col + 128] = rounded
                    rest = rest - rounded.astype(jnp.float32)

    whole = pl.BlockSpec(memory_space=pltpu.VMEM)
    scalar = pl.BlockSpec(memory_space=pltpu.SMEM)
    outs = pl.pallas_call(
        kernel,
        out_shape=[jax.ShapeDtypeStruct((rows + extra, head_width), jnp.bfloat16)] * sources,
        in_specs=[scalar, scalar] + [whole] * (sources + 2),
        out_specs=[whole] * sources,
        scratch_shapes=[
            pltpu.SMEM((slots,), jnp.int32),
            pltpu.SMEM((slots,), jnp.int32),
            pltpu.VMEM((slots, head_width // 128, block_len, 128), jnp.bfloat16),
            pltpu.VMEM((slots, heads, block_len, 128), jnp.float32),
            pltpu.VMEM((slots, heads, block_len, 128), jnp.float32),
            pltpu.VMEM((slots, heads, block_len, pass_rows), jnp.bfloat16),
        ],
        name="owner_attention",
    )(me, ids, *query_list, keys, values)
    return outs


def merge_owners(out_list, rows):
    sources = len(out_list)
    head_width = out_list[0].shape[1]
    heads = head_width // HD
    places, _ = stat_place(rows, head_width)

    def kernel(*refs):
        out_refs = refs[:sources]
        result_ref = refs[sources]
        for at in range(0, rows, 128):
            stats = []
            for ref in out_refs:
                pieces = []
                for piece in range(3):
                    row, col = places[piece * (rows // 128) + at // 128]
                    pieces.append(ref[row : row + 8, col : col + 128].astype(jnp.float32))
                stats.append(pieces[2] + pieces[1] + pieces[0])
            best = [stats[0][h : h + 1] for h in range(heads)]
            for s in range(1, sources):
                best = [jnp.maximum(best[h], stats[s][h : h + 1]) for h in range(heads)]
            weights = [
                [jnp.exp(stats[s][h : h + 1] - best[h]) for h in range(heads)]
                for s in range(sources)
            ]
            for h in range(heads):
                total = weights[0][h] * stats[0][heads + h : heads + h + 1]
                for s in range(1, sources):
                    total = total + weights[s][h] * stats[s][heads + h : heads + h + 1]
                table = jnp.concatenate(
                    [weights[s][h] / total for s in range(sources)]
                    + [jnp.zeros((128 - sources, 128), jnp.float32)],
                    axis=0,
                ).T
                cols = slice(h * HD, (h + 1) * HD)
                merged = jnp.zeros((128, HD), jnp.float32)
                for s in range(sources):
                    merged = merged + table[:, s : s + 1] * out_refs[s][
                        at : at + 128, cols
                    ].astype(jnp.float32)
                result_ref[at : at + 128, cols] = merged.astype(jnp.bfloat16)

    whole = pl.BlockSpec(memory_space=pltpu.VMEM)
    return pl.pallas_call(
        kernel,
        out_shape=jax.ShapeDtypeStruct((rows, head_width), jnp.bfloat16),
        in_specs=[whole] * sources,
        out_specs=whole,
        name="merge_owners",
    )(*out_list)


def local(
    tokens,
    store,
    passage_ids,
    mix_gain,
    glu_value,
    glu_gate,
    conv_taps,
    channel_gain,
    mix_out,
    query_gain,
    passage_gain,
    query_proj,
    key_proj,
    value_proj,
    attn_out,
    blend_gain,
):
    owners = lax.axis_size("st")
    shards = lax.axis_size("tp")
    me = lax.axis_index("st").astype(jnp.int32)
    mine = lax.axis_index("tp")
    tok_rows, model_width = tokens.shape
    local_channels = glu_value.shape[1]
    head_width = query_proj.shape[1]
    block_count, per_block = passage_ids.shape
    block_len = tok_rows // block_count
    pass_local, pass_rows, _ = store.shape
    blocks_per_shard = block_count // shards
    chunks = CHUNKS if blocks_per_shard % CHUNKS == 0 else 1
    run = blocks_per_shard // chunks * block_len
    steps = range(1, owners)

    def cut(rows, c):
        return rows.reshape(shards, chunks, run, -1)[:, c].reshape(shards * run, -1)

    queries = jnp.dot(
        rms_rows(tokens, query_gain), query_proj, preferred_element_type=jnp.float32
    ).astype(jnp.bfloat16)
    assert owners * pass_local <= 256
    query_chunks = []
    id_chunks = []
    for c in range(chunks):
        ids = passage_ids.reshape(shards, chunks, -1)[:, c].reshape(1, -1)
        id_rows = jnp.pad(
            ids.astype(jnp.bfloat16), ((0, 15), (0, head_width - ids.shape[1]))
        )
        own = jnp.concatenate([cut(queries, c), id_rows], axis=0)
        query_list = [own] + [shifted(own, "st", k) for k in steps]
        query_chunks.append(query_list)
        id_chunks.append(
            jnp.stack([q[shards * run, : ids.shape[1]] for q in query_list]).astype(jnp.int32)
        )
    key_planes, value_planes = passage_planes(
        store.reshape(pass_local * pass_rows, model_width), passage_gain, key_proj, value_proj
    )
    mix_input = rms_rows(tokens, mix_gain)
    value_part = jnp.dot(mix_input, glu_value, preferred_element_type=jnp.float32)
    gate_part = jnp.dot(mix_input, glu_gate, preferred_element_type=jnp.float32)
    gated_rows = (value_part * jax.nn.sigmoid(gate_part)).astype(jnp.bfloat16)
    conv_rows = depthwise(gated_rows.reshape(-1, SEQ_LEN, local_channels), conv_taps).reshape(
        tok_rows, local_channels
    )
    sums = jnp.stack([jnp.sum(conv_rows, axis=1), jnp.sum(conv_rows * conv_rows, axis=1)])
    channel_total = sums
    for k in range(1, shards):
        channel_total = channel_total + shifted(sums, "tp", k)
    answers = []
    for c in range(chunks):
        out_list = owner_attention(
            me[None],
            id_chunks[c],
            query_chunks[c],
            key_planes,
            value_planes,
            block_len,
            per_block,
            pass_rows,
        )
        answers.append([out_list[0]] + [shifted(out_list[k], "st", -k) for k in steps])
    row_mean = channel_total[0] / CA
    row_var = channel_total[1] / CA - row_mean * row_mean
    activation = jax.nn.silu(
        (conv_rows - row_mean[:, None]) * lax.rsqrt(row_var + EPS)[:, None] * channel_gain
    ).astype(jnp.bfloat16)
    results = []
    for c in range(chunks):
        attended = merge_owners(answers[c], shards * run)
        conv_term = jnp.dot(cut(activation, c), mix_out, preferred_element_type=jnp.float32)
        attn_term = jnp.dot(attended, attn_out, preferred_element_type=jnp.float32)
        partial = (
            (conv_term + blend_gain * attn_term).astype(jnp.bfloat16).reshape(shards, run, -1)
        )
        order = sorted(range(1, shards), key=lambda k: -min(k, shards - k))
        pieces = [
            shifted(
                lax.dynamic_index_in_dim(partial, (mine + k) % shards, 0, keepdims=False),
                "tp",
                k,
            )
            for k in order
        ]
        total = lax.dynamic_index_in_dim(partial, mine, 0, keepdims=False).astype(jnp.float32)
        for piece in pieces:
            total = total + piece.astype(jnp.float32)
        results.append(total.astype(jnp.bfloat16))
    return jnp.concatenate(results, axis=0)


CHUNKS = 2


def solution(mesh):
    in_specs = (
        P(("grp", "st"), None),
        P(("grp", "st"), None, None),
        P(("grp", "st"), None),
        P(),
        P(None, "tp"),
        P(None, "tp"),
        P(None, "tp"),
        P("tp"),
        P("tp", None),
        P(),
        P(),
        P(None, "tp"),
        P(None, "tp"),
        P(None, "tp"),
        P("tp", None),
        P(),
    )
    out_specs = P(("grp", "st", "tp"), None)
    return jax.shard_map(local, mesh=mesh, in_specs=in_specs, out_specs=out_specs, check_vma=False)
```
